32 devices in a mesh: sp: 16 (over z, y, core), tp: 2 (over x).
Axes of the slice: x: 2, y: 2, z: 4, core: 2. Of those that a mesh axis runs over, the one named last changes fastest.
Arguments:
- tokens: bfloat16 [1, 8192, 2048], P(None, ('sp', 'tp')), may hold values from -6 to 6
- input_norm_gain: float32 [2048], replicated, may hold values from 0.1 to 1.9
- query_weight: bfloat16 [2048, 1024], P(None, 'tp'), may hold values from -0.125 to 0.125
- forget_weight: bfloat16 [2048, 1024], P(None, 'tp'), may hold values from -0.125 to 0.125
- input_weight: bfloat16 [2048, 1024], P(None, 'tp'), may hold values from -0.125 to 0.125
- gate_weight: bfloat16 [2048, 1024], P(None, 'tp'), may hold values from -0.125 to 0.125
- slack: float32 [1024], P('tp'), may hold values from 0 to 0.06
- sudden_decay: float32 [1, 8192, 8], P(None, 'sp', 'tp'), may hold values from -0.75 to 0
- head_norm_gain: float32 [128], replicated, may hold values from 0.1 to 1.9
- output_weight: bfloat16 [1024, 2048], P(None, 'tp'), may hold values from -1.25 to 1.25
- output_norm_gain: float32 [2048], P('tp'), may hold values from 0.1 to 1.9
Outputs:
- mixer_output: bfloat16 [1, 8192, 2048], P(None, 'sp', 'tp')
The draws below stay inside these ranges and needn't reach their ends.
All inputs are finite; a program needn't handle non-finite values.
Results may differ from the reference program's by a relative error of at most 0.0094.
Values may be sent and summed in bfloat16 or wider, within the bound.
A program may use at most 64 MiB of HBM per device.

```python
import math
import jax
import jax.numpy as jnp
from jax import lax

D = 2048
HEADS = 8
KEY = 128
VAL = 128
BLOCK = 64
SEQUENCE_COUNT = 1
TOKENS_PER_SHARD = 512
SEQUENCE_LENGTH = 8192


def head_plan(key):
    head_order = jax.random.permutation(jax.random.fold_in(key, 101), HEADS)
    fast_count = HEADS // 2
    return head_order < fast_count


def spread_draw(key, lowest, highest, extent):
    return jnp.exp(jax.random.uniform(key, extent, jnp.float32, math.log(lowest), math.log(highest)))


def draw_slack(key, part):
    fast_heads = head_plan(key)
    quick_rate = spread_draw(jax.random.fold_in(key, 1), 0.02, 0.06, (HEADS, KEY))
    slow_rate = spread_draw(jax.random.fold_in(key, 2), 0.2 / SEQUENCE_LENGTH, 0.6 / SEQUENCE_LENGTH, (HEADS, KEY))
    return jnp.where(fast_heads[:, None], quick_rate, slow_rate).reshape(HEADS * KEY).astype(jnp.float32)


def draw_sudden_decay(key, part):
    fast_heads = head_plan(key)
    per_head_rate = jnp.where(fast_heads, spread_draw(jax.random.fold_in(key, 3), 0.005, 0.02, (HEADS,)), spread_draw(jax.random.fold_in(key, 4), 0.2 / SEQUENCE_LENGTH, 0.5 / SEQUENCE_LENGTH, (HEADS,)))
    multiplier = spread_draw(jax.random.fold_in(key, 5), 0.25, 2.0, (SEQUENCE_COUNT, SEQUENCE_LENGTH // TOKENS_PER_SHARD))
    multiplier = jnp.repeat(multiplier, TOKENS_PER_SHARD, axis=1)
    sudden_positions = jax.random.randint(jax.random.fold_in(key, 6), (SEQUENCE_COUNT, 2), 0, SEQUENCE_LENGTH)
    sudden_loss = jax.random.uniform(jax.random.fold_in(key, 7), (SEQUENCE_COUNT, 2), jnp.float32, 0.2, 0.5)
    locations = jnp.arange(SEQUENCE_LENGTH)[None, :, None]
    sudden_drops = jnp.sum(jnp.where(locations == sudden_positions[:, None, :], jnp.log(1.0 - sudden_loss)[:, None, :], 0.0), axis=2)
    return (sudden_drops[:, :, None] - per_head_rate[None, None, :] * multiplier[:, :, None]).astype(jnp.float32)


def draw_output_weight(key, part):
    columns = jnp.arange(D, dtype=jnp.float32) / D
    jitter = jax.random.uniform(jax.random.fold_in(key, 8), (D,), jnp.float32)
    exponent = 0.5 * columns + 0.5 * jitter
    entries = jax.random.truncated_normal(jax.random.fold_in(key, 9), -4.0, 4.0, (HEADS * VAL, D), jnp.float32)
    return (entries * (10.0 ** exponent)[None, :] * (HEADS * VAL) ** (-0.5)).astype(jnp.bfloat16)


def shard_levels(own_key, shape, cuts, least, largest):
    factor_of = 1.0
    for axis_at, parts in cuts:
        steps = jax.random.uniform(jax.random.fold_in(jax.random.fold_in(own_key, 6), axis_at), (parts,), jnp.float32, least / len(cuts), largest / len(cuts))
        factor_of = factor_of * jnp.repeat(jnp.exp(steps), shape[axis_at] // parts).reshape((-1,) + (1,) * (len(shape) - 1 - axis_at))
    return factor_of


def gaussian(stream_key, dims, spread, most, cuts=(), held_as=jnp.bfloat16):
    array = spread * jax.random.normal(stream_key, dims, jnp.float32)
    if cuts:
        array = array * shard_levels(stream_key, dims, cuts, -0.22, 0.18)
    return jnp.clip(array, -most, most).astype(held_as)


def setup_inputs(seed: int = 0) -> dict:
    splits = jax.random.split(jax.random.key(seed), 12)
    return {
        "tokens": gaussian(splits[0], (SEQUENCE_COUNT, SEQUENCE_LENGTH, D), 1.0, 6.0, ((1, 32),)),
        "input_norm_gain": jnp.clip(1.0 + 0.18 * jax.random.normal(splits[1], (D,), jnp.float32), 0.1, 1.9),
        "query_weight": gaussian(splits[2], (D, HEADS * KEY), D ** -0.5, 0.125, ((1, 2),)),
        "forget_weight": gaussian(splits[3], (D, HEADS * KEY), D ** -0.5, 0.125, ((1, 2),)),
        "input_weight": gaussian(splits[4], (D, HEADS * VAL), D ** -0.5, 0.125, ((1, 2),)),
        "gate_weight": gaussian(splits[5], (D, HEADS * VAL), D ** -0.5, 0.125, ((1, 2),)),
        "slack": draw_slack(jax.random.fold_in(splits[11], 71), 0),
        "sudden_decay": draw_sudden_decay(jax.random.fold_in(splits[11], 71), 0),
        "head_norm_gain": jnp.clip(1.0 + 0.18 * jax.random.normal(splits[8], (VAL,), jnp.float32), 0.1, 1.9),
        "output_weight": draw_output_weight(jax.random.fold_in(splits[11], 71), 0),
        "output_norm_gain": jnp.clip(1.0 + 0.18 * jax.random.normal(splits[10], (D,), jnp.float32), 0.1, 1.9),
    }


epsilon = 1e-06
precise = lax.Precision.HIGHEST

def normalize(tensor_in, gain_vec):
    tensor_in = tensor_in.astype(jnp.float32)
    return tensor_in * lax.rsqrt(lax.optimization_barrier(jnp.mean(tensor_in * tensor_in, axis=-1, keepdims=True)) + epsilon) * gain_vec

def setup_params(query_logits, forget_logits, input_logits, slack, sudden_decay):
    sequence_total, sequence_span, local_heads = sudden_decay.shape

    def heads_first(tensor):
        return tensor.astype(jnp.float32).reshape(sequence_total, sequence_span, local_heads, -1).transpose(0, 2, 1, 3)
    query_rows = heads_first(query_logits) * KEY ** (-0.5)
    incoming_weights = slack.reshape(local_heads, -1)[None, :, None, :] * jax.nn.sigmoid(-heads_first(forget_logits))
    forget_logarithm = jnp.log1p(-incoming_weights) + sudden_decay.transpose(0, 2, 1)[:, :, :, None]
    return (query_rows, incoming_weights, heads_first(input_logits), forget_logarithm)

def block_pass(query_rows, incoming_weights, value_rows, forget_logarithm, initial):
    sequence_total, local_heads, sequence_span, key_width = query_rows.shape
    blocks_here = sequence_span // BLOCK

    def by_block(tensor):
        return tensor.reshape(sequence_total, local_heads, blocks_here, BLOCK, tensor.shape[3]).transpose(2, 0, 1, 3, 4)
    causal = jnp.tril(jnp.ones((BLOCK, BLOCK), dtype=bool))

    def advance(carried, portions):
        query_blk, weight_blk, value_blk, forget_blk = portions
        running = jnp.cumsum(forget_blk, axis=2)
        lifted_q = query_blk * jnp.exp(running)
        lifted_k = weight_blk * jnp.exp(-running)
        scores = jnp.einsum('shtk,shuk->shtu', lifted_q, lifted_k, precision=precise)
        scores = jnp.where(causal, scores, 0.0)
        produced = jnp.einsum('shtu,shuv->shtv', scores, value_blk, precision=precise) + jnp.einsum('shtk,shkv->shtv', lifted_q, carried, precision=precise)
        ending = running[:, :, -1:, :]
        carried = jnp.exp(ending[:, :, 0, :])[..., None] * carried + jnp.einsum('shuk,shuv->shkv', weight_blk * jnp.exp(ending - running), value_blk, precision=precise)
        return (carried, produced)
    final_state, produced = lax.scan(advance, initial, (by_block(query_rows), by_block(incoming_weights), by_block(value_rows), by_block(forget_logarithm)))
    return (final_state, produced.transpose(1, 2, 0, 3, 4).reshape(sequence_total, local_heads, sequence_span, value_rows.shape[3]))

def gate_heads(produced, gate_raw, head_norm_gain):
    sequence_total, local_heads, sequence_span, val_width = produced.shape
    mean_sq = lax.optimization_barrier(jnp.mean(produced * produced, axis=3, keepdims=True))
    scaled = produced * lax.rsqrt(mean_sq + epsilon) * head_norm_gain
    scaled = scaled.transpose(0, 2, 1, 3).reshape(sequence_total, sequence_span, local_heads * val_width)
    return (scaled * jax.nn.silu(gate_raw.astype(jnp.float32))).astype(jnp.bfloat16)

def reference(tokens, input_norm_gain, query_weight, forget_weight, input_weight, gate_weight, slack, sudden_decay, head_norm_gain, output_weight, output_norm_gain):
    sequence_total, sequence_span, model_width = tokens.shape
    matrices = [matrix.astype(jnp.float32) for matrix in (query_weight, forget_weight, input_weight, gate_weight)]
    out_matrix = output_weight.astype(jnp.float32)
    segments = sequence_span // TOKENS_PER_SHARD

    def segment(carried, seg_index):
        leading_row = (seg_index * TOKENS_PER_SHARD).astype(jnp.int32)
        token_rows = lax.dynamic_slice_in_dim(tokens, leading_row, TOKENS_PER_SHARD, 1)
        normed = normalize(token_rows, input_norm_gain).astype(jnp.bfloat16)
        normed = lax.optimization_barrier(normed).astype(jnp.float32)
        unprocessed_parts = [lax.optimization_barrier(jnp.einsum('std,dc->stc', normed, matrix).astype(jnp.bfloat16)) for matrix in matrices]
        sudden_rows = lax.dynamic_slice_in_dim(sudden_decay, leading_row, TOKENS_PER_SHARD, 1)
        query_rows, incoming_weights, value_rows, forget_logarithm = setup_params(unprocessed_parts[0], unprocessed_parts[1], unprocessed_parts[2], slack, sudden_rows)
        carried, produced = block_pass(query_rows, incoming_weights, value_rows, forget_logarithm, carried)
        gated_out = lax.optimization_barrier(gate_heads(produced, unprocessed_parts[3], head_norm_gain)).astype(jnp.float32)
        projected = jnp.einsum('stc,cd->std', gated_out, out_matrix)
        return (carried, normalize(projected, output_norm_gain).astype(jnp.bfloat16))
    initial = jnp.zeros((sequence_total, HEADS, KEY, VAL), jnp.float32)
    _, outputs = lax.scan(segment, initial, jnp.arange(segments, dtype=jnp.int32))
    return outputs.transpose(1, 0, 2, 3).reshape(sequence_total, sequence_span, model_width)
```

```python
import functools

import jax
import jax.numpy as jnp
from jax import lax
from jax.experimental import pallas as pl
from jax.experimental.pallas import tpu as pltpu
from jax.sharding import PartitionSpec as P

KEY = 128
EPS = 1e-06
MESH = pl.DeviceIdType.MESH
F32 = jnp.float32
BF16 = jnp.bfloat16


def dot(a, b, dims=((1,), (0,))):
    return lax.dot_general(a, b, (dims, ((), ())), preferred_element_type=F32)


def kernel(
    cfg,
    tokens, gain, wq, wf, wi, wg, slack, sudden, head_gain, wo, out_gain,
    out,
    raw, w, ow, states, inner, lifted, gates, mids, cums, gated, proj,
    mine, theirs, tx, rx, inc_s, inc_d, exc_s, exc_d, ex_tx, ex_rx, entry,
    squares,
    w_sem, own_sem, raw_send, raw_recv, pair_send, pair_recv, ks_send, ks_recv,
    ex_send, ex_recv, g_send, g_recv, s_send, s_recv,
):
    n_sp, n_tp, seg, block, heads, model = cfg
    rows_all = seg * n_tp
    blocks = rows_all // block
    per_seg = seg // block
    hk = heads * KEY
    half = hk // 2
    chips = n_sp // 2
    steps = []
    d = 1
    while d < chips:
        steps.append(d)
        d *= 2
    p = lax.axis_index("sp")
    t = lax.axis_index("tp")
    core = lax.rem(p, 2)
    chip = p // 2
    partner = p + 1 - 2 * core

    for at, ref in enumerate((wq, wf, wi, wg)):
        pltpu.make_async_copy(ref, w.at[at], w_sem.at[at]).start()
    own_rows = pl.ds(pl.multiple_of(t * seg, seg), seg)
    own_copy = pltpu.make_async_copy(tokens, raw.at[own_rows], own_sem)
    own_copy.start()
    pltpu.make_async_copy(wo, ow, w_sem.at[4]).start()

    barrier = pltpu.get_barrier_semaphore()

    def greet(sp_at, tp_at):
        pl.semaphore_signal(barrier, inc=1, device_id=(sp_at, tp_at), device_id_type=MESH)

    for k in range(1, n_tp):
        greet(p, lax.rem(t + k, n_tp))
    greet(partner, t)
    for d in steps:
        @pl.when(chip + d < chips)
        def _():
            greet(p + 2 * d, t)

        @pl.when(chip >= d)
        def _():
            greet(p - 2 * d, t)
    peers = n_tp
    for d in steps:
        peers = peers + jnp.where(chip + d < chips, 1, 0) + jnp.where(chip >= d, 1, 0)
    pl.semaphore_wait(barrier, peers)

    def raw_copy(k, i, source):
        at = pl.ds(pl.multiple_of(source * seg + i * block, block), block)
        return pltpu.make_async_remote_copy(
            src_ref=tokens.at[pl.ds(i * block, block)],
            dst_ref=raw.at[at],
            send_sem=raw_send.at[k - 1, i],
            recv_sem=raw_recv.at[k - 1, i],
            device_id=(p, lax.rem(t + k, n_tp)),
            device_id_type=MESH,
        )

    for i in range(per_seg):
        for k in range(1, n_tp):
            raw_copy(k, i, t).start()

    row = lax.broadcasted_iota(jnp.int32, (block, block), 0)
    col = lax.broadcasted_iota(jnp.int32, (block, block), 1)
    causal = col <= row
    mid = block // 2 - 1
    sums = jnp.where(
        (col > mid) & (col <= row), 1.0, jnp.where((col <= mid) & (col > row), -1.0, 0.0)
    ).astype(BF16)

    def process(b):
        rows = pl.ds(pl.multiple_of(b * block, block), block)
        x = raw[rows, :].astype(F32)
        scale = lax.rsqrt(jnp.mean(x * x, axis=1, keepdims=True) + EPS)
        normed = (x * scale * gain[...]).astype(BF16)
        fr = dot(normed, w[1]).astype(BF16).astype(F32)
        values = dot(normed, w[2]).astype(BF16)
        weight = slack[...] / (1.0 + jnp.exp(fr))
        sd = sudden[rows, :]
        sd = jnp.concatenate(
            [jnp.broadcast_to(sd[:, h : h + 1], (block, KEY)) for h in range(heads)], axis=1
        )
        logs = jnp.log1p(-weight) + sd
        high = logs.astype(BF16)
        low = (logs - high.astype(F32)).astype(BF16)
        centred = dot(sums, high) + dot(sums, low)
        ending = centred[block - 1 : block, :]
        to_mid = logs[0:1, :] - centred[0:1, :]
        lifted_k = weight * jnp.exp(-centred)
        kept = (lifted_k * jnp.exp(ending)).astype(BF16)
        lifted_k = lifted_k.astype(BF16)
        mids[b] = jnp.broadcast_to(to_mid, (8, hk))
        cums[b] = jnp.broadcast_to(to_mid + ending, (8, hk))
        for h in range(heads):
            at = slice(h * KEY, (h + 1) * KEY)
            states[b, :, at] = dot(values[:, at], kept[:, at], ((0,), (0,)))
        qr = dot(normed, w[0]).astype(BF16).astype(F32) * KEY ** (-0.5)
        lifted_q = (qr * jnp.exp(centred)).astype(BF16)
        lifted[rows, :] = lifted_q
        gates[rows, :] = dot(normed, w[3]).astype(BF16)
        for h in range(heads):
            at = slice(h * KEY, (h + 1) * KEY)
            scores = dot(lifted_q[:, at], lifted_k[:, at], ((1,), (1,)))
            scores = jnp.where(causal, scores, 0.0).astype(BF16)
            inner[rows, at] = dot(scores, values[:, at])

    own_copy.wait()
    for at, ref in enumerate((wq, wf, wi, wg)):
        pltpu.make_async_copy(ref, w.at[at], w_sem.at[at]).wait()

    def own_block(i, carry):
        process(t * per_seg + i)
        return carry

    lax.fori_loop(0, per_seg, own_block, 0)
    for i in range(per_seg):
        for k in range(1, n_tp):
            source = lax.rem(t + n_tp - k, n_tp)
            raw_copy(k, i, source).wait_recv()
            process(source * per_seg + i)

    state = jnp.zeros((KEY, hk), F32)
    total = jnp.zeros((1, hk), F32)
    for b in range(blocks):
        fresh = states[b]
        step_log = cums[b][0:1, :]
        states[b] = state
        cums[b] = jnp.broadcast_to(total, (8, hk))
        state = jnp.exp(step_log) * state + fresh
        total = total + step_log
    decay = jnp.exp(total)

    def fill(ref, s, dec):
        width = dec.shape[1]
        ref[0:KEY, :] = s.astype(BF16)
        hi = dec.astype(BF16).astype(F32)
        lo = dec - hi
        at = lax.broadcasted_iota(jnp.int32, (16, width), 0)
        tail = jnp.where(at == 0, hi, jnp.where(at == 1, lo, 0.0))
        ref[KEY : KEY + 16, :] = tail.astype(BF16)

    def read(ref):
        s = ref[0:KEY, :].astype(F32)
        tail = ref[KEY : KEY + 16, :].astype(F32)
        return s, tail[0:1, :] + tail[1:2, :]

    fill(mine, state, decay)
    pair = pltpu.make_async_remote_copy(
        src_ref=mine, dst_ref=theirs, send_sem=pair_send, recv_sem=pair_recv,
        device_id=(partner, t), device_id_type=MESH,
    )
    pair.start()
    pair.wait_recv()
    their_s, their_d = read(theirs)
    first = core == 0
    joined_s = jnp.where(first, their_d * state + their_s, decay * their_s + state)
    joined_d = decay * their_d
    inc_s[...] = jnp.where(first, joined_s[:, :half], joined_s[:, half:])
    inc_d[...] = jnp.broadcast_to(
        jnp.where(first, joined_d[:, :half], joined_d[:, half:]), (8, half)
    )
    exc_s[...] = jnp.zeros_like(exc_s)
    exc_d[...] = jnp.ones_like(exc_d)

    def ks_copy(k, to):
        return pltpu.make_async_remote_copy(
            src_ref=tx.at[k], dst_ref=rx.at[k], send_sem=ks_send.at[k], recv_sem=ks_recv.at[k],
            device_id=(to, t), device_id_type=MESH,
        )

    for k, d in enumerate(steps):
        @pl.when(chip + d < chips)
        def _():
            fill(tx.at[k], inc_s[...], inc_d[0:1, :])
            ks_copy(k, p + 2 * d).start()

        @pl.when(chip >= d)
        def _():
            ks_copy(k, p).wait_recv()
            got_s, got_d = read(rx.at[k])
            exc_s[...] = exc_d[0:1, :] * got_s + exc_s[...]
            exc_d[...] = exc_d[...] * got_d
            if k < len(steps) - 1:
                inc_s[...] = inc_d[0:1, :] * got_s + inc_s[...]
                inc_d[...] = inc_d[...] * got_d

    ex_tx[...] = exc_s[...].astype(BF16)
    swap = pltpu.make_async_remote_copy(
        src_ref=ex_tx, dst_ref=ex_rx, send_sem=ex_send, recv_sem=ex_recv,
        device_id=(partner, t), device_id_type=MESH,
    )
    swap.start()
    swap.wait_recv()
    own_half = exc_s[...]
    other_half = ex_rx[...].astype(F32)
    both = jnp.concatenate(
        [jnp.where(first, own_half, other_half), jnp.where(first, other_half, own_half)], axis=1
    )
    their_s, their_d = read(theirs)
    entry[...] = jnp.where(first, both, their_d * both + their_s)

    def g_copy(k, b, source):
        rows = pl.ds(pl.multiple_of(b * block, block), block)
        return pltpu.make_async_remote_copy(
            src_ref=gated.at[t, rows],
            dst_ref=gated.at[source, rows],
            send_sem=g_send.at[k - 1, b],
            recv_sem=g_recv.at[k - 1, b],
            device_id=(p, lax.rem(t + k, n_tp)),
            device_id_type=MESH,
        )

    def finish(b, carry):
        rows = pl.ds(pl.multiple_of(b * block, block), block)
        at_start = jnp.exp(mids[b][0:1, :]) * (
            states[b] + jnp.exp(cums[b][0:1, :]) * entry[...]
        )
        at_start = at_start.astype(BF16)
        for h in range(heads):
            at = slice(h * KEY, (h + 1) * KEY)
            whole = inner[rows, at] + dot(lifted[rows, at], at_start[:, at], ((1,), (1,)))
            scale = lax.rsqrt(jnp.mean(whole * whole, axis=1, keepdims=True) + EPS)
            g = gates[rows, at].astype(F32)
            result = whole * scale * head_gain[...] * (g / (1.0 + jnp.exp(-g)))
            gated[t, rows, at] = result.astype(BF16)
        for k in range(1, n_tp):
            g_copy(k, b, t).start()
        return carry

    lax.fori_loop(0, blocks, finish, 0)

    def s_copy(k, b, source):
        return pltpu.make_async_remote_copy(
            src_ref=squares.at[t, b],
            dst_ref=squares.at[source, b],
            send_sem=s_send.at[k - 1, b],
            recv_sem=s_recv.at[k - 1, b],
            device_id=(p, lax.rem(t + k, n_tp)),
            device_id_type=MESH,
        )

    pltpu.make_async_copy(wo, ow, w_sem.at[4]).wait()

    def project(b, carry):
        rows = pl.ds(pl.multiple_of(b * block, block), block)
        for k in range(1, n_tp):
            g_copy(k, b, lax.rem(t + n_tp - k, n_tp)).wait_recv()
        acc = dot(gated[0, rows, :], ow[0:hk, :])
        for j in range(1, n_tp):
            acc = acc + dot(gated[j, rows, :], ow[j * hk : (j + 1) * hk, :])
        proj[rows, :] = acc
        line = jnp.sum(acc * acc, axis=1, keepdims=True)
        square = jnp.transpose(jnp.broadcast_to(line, (block, 128)))
        squares[t, b] = square[0:8, :]
        for k in range(1, n_tp):
            s_copy(k, b, t).start()
        return carry

    lax.fori_loop(0, blocks, project, 0)

    def close(b, carry):
        rows = pl.ds(pl.multiple_of(b * block, block), block)
        for k in range(1, n_tp):
            s_copy(k, b, lax.rem(t + n_tp - k, n_tp)).wait_recv()
        line = squares[0, b][0:1, :]
        for j in range(1, n_tp):
            line = line + squares[j, b][0:1, :]
        column = jnp.transpose(jnp.broadcast_to(line, (128, block)))[:, 0:1]
        out[rows, :] = (
            proj[rows, :] * lax.rsqrt(column * (1.0 / model) + EPS) * out_gain[...]
        ).astype(BF16)
        return carry

    lax.fori_loop(0, blocks, close, 0)

    for i in range(per_seg):
        for k in range(1, n_tp):
            raw_copy(k, i, t).wait_send()
    pair.wait_send()
    for k, d in enumerate(steps):
        @pl.when(chip + d < chips)
        def _():
            ks_copy(k, p + 2 * d).wait_send()
    swap.wait_send()
    for b in range(blocks):
        for k in range(1, n_tp):
            g_copy(k, b, t).wait_send()
            s_copy(k, b, t).wait_send()


def solution(mesh):
    n_sp, n_tp = mesh.shape["sp"], mesh.shape["tp"]

    def shards(tokens, gain, wq, wf, wi, wg, slack, sudden, head_gain, wo, out_gain):
        seg, model = tokens.shape[1:]
        hk = wq.shape[1]
        heads = hk // KEY
        features = wo.shape[1]
        rows_all = seg * n_tp
        block = min(128, seg)
        blocks = rows_all // block
        per_seg = seg // block
        half = hk // 2
        chips = n_sp // 2
        steps = max(1, (chips - 1).bit_length())
        peers = n_tp - 1
        any_spec = pl.BlockSpec(memory_space=pl.ANY)
        vmem = pl.BlockSpec(memory_space=pltpu.VMEM)
        dma = pltpu.SemaphoreType.DMA
        cfg = (n_sp, n_tp, seg, block, heads, model)
        call = pl.pallas_call(
            functools.partial(kernel, cfg),
            out_shape=jax.ShapeDtypeStruct((rows_all, features), BF16),
            in_specs=[
                any_spec, vmem, any_spec, any_spec, any_spec, any_spec,
                vmem, vmem, vmem, any_spec, vmem,
            ],
            out_specs=vmem,
            scratch_shapes=[
                pltpu.VMEM((rows_all, model), BF16),
                pltpu.VMEM((4, model, hk), BF16),
                pltpu.VMEM((hk * n_tp, features), BF16),
                pltpu.VMEM((blocks, KEY, hk), F32),
                pltpu.VMEM((rows_all, hk), F32),
                pltpu.VMEM((rows_all, hk), BF16),
                pltpu.VMEM((rows_all, hk), BF16),
                pltpu.VMEM((blocks, 8, hk), F32),
                pltpu.VMEM((blocks, 8, hk), F32),
                pltpu.VMEM((n_tp, rows_all, hk), BF16),
                pltpu.VMEM((rows_all, features), F32),
                pltpu.VMEM((KEY + 16, hk), BF16),
                pltpu.VMEM((KEY + 16, hk), BF16),
                pltpu.VMEM((steps, KEY + 16, half), BF16),
                pltpu.VMEM((steps, KEY + 16, half), BF16),
                pltpu.VMEM((KEY, half), F32),
                pltpu.VMEM((8, half), F32),
                pltpu.VMEM((KEY, half), F32),
                pltpu.VMEM((8, half), F32),
                pltpu.VMEM((KEY, half), BF16),
                pltpu.VMEM((KEY, half), BF16),
                pltpu.VMEM((KEY, hk), F32),
                pltpu.VMEM((n_tp, blocks, 8, 128), F32),
                dma((5,)), dma,
                dma((peers, per_seg)), dma((peers, per_seg)),
                dma, dma,
                dma((steps,)), dma((steps,)),
                dma, dma,
                dma((peers, blocks)), dma((peers, blocks)),
                dma((peers, blocks)), dma((peers, blocks)),
            ],
            compiler_params=pltpu.CompilerParams(
                collective_id=0, has_side_effects=True, vmem_limit_bytes=60 * 2**20
            ),
        )
        result = call(
            tokens[0], gain[None], wq, wf, wi, wg, slack[None], sudden[0],
            head_gain[None], wo, out_gain[None],
        )
        return result[None]

    placed = (
        P(None, ("sp", "tp"), None),
        P(),
        P(None, "tp"),
        P(None, "tp"),
        P(None, "tp"),
        P(None, "tp"),
        P("tp"),
        P(None, "sp", "tp"),
        P(),
        P(None, "tp"),
        P("tp"),
    )
    return jax.shard_map(
        shards, mesh=mesh, in_specs=placed, out_specs=P(None, "sp", "tp"), check_vma=False
    )
```

```python
import functools

import jax
import jax.numpy as jnp
from jax import lax
from jax.experimental import pallas as pl
from jax.experimental.pallas import tpu as pltpu
from jax.sharding import PartitionSpec as P

KEY = 128
EPS = 1e-06
MESH = pl.DeviceIdType.MESH
F32 = jnp.float32
BF16 = jnp.bfloat16


def dot(a, b, dims=((1,), (0,))):
    return lax.dot_general(a, b, (dims, ((), ())), preferred_element_type=F32)


def kernel(
    cfg,
    tokens, gain, wq, wf, wi, wg, slack, sudden, head_gain, wo, out_gain,
    out,
    raw, w, ow, states, inner, lifted, gates, mids, cums, gated, proj, centres, keys, vals, normal,
    mine, theirs, tx, rx, inc_s, inc_d, exc_s, exc_d, ex_tx, ex_rx, entry,
    squares,
    w_sem, own_sem, raw_send, raw_recv, pair_send, pair_recv, ks_send, ks_recv,
    ex_send, ex_recv, g_send, g_recv, s_send, s_recv,
):
    n_sp, n_tp, seg, block, heads, model = cfg
    rows_all = seg * n_tp
    blocks = rows_all // block
    per_seg = seg // block
    hk = heads * KEY
    half = hk // 2
    chips = n_sp // 2
    steps = []
    d = 1
    while d < chips:
        steps.append(d)
        d *= 2
    p = lax.axis_index("sp")
    t = lax.axis_index("tp")
    core = lax.rem(p, 2)
    chip = p // 2
    partner = p + 1 - 2 * core

    for at, ref in enumerate((wq, wf, wi, wg)):
        pltpu.make_async_copy(ref, w.at[at], w_sem.at[at]).start()
    own_rows = pl.ds(pl.multiple_of(t * seg, seg), seg)
    own_copy = pltpu.make_async_copy(tokens, raw.at[own_rows], own_sem)
    own_copy.start()
    pltpu.make_async_copy(wo, ow, w_sem.at[4]).start()

    barrier = pltpu.get_barrier_semaphore()

    def greet(sp_at, tp_at):
        pl.semaphore_signal(barrier, inc=1, device_id=(sp_at, tp_at), device_id_type=MESH)

    for k in range(1, n_tp):
        greet(p, lax.rem(t + k, n_tp))
    greet(partner, t)
    for d in steps:
        @pl.when(chip + d < chips)
        def _():
            greet(p + 2 * d, t)

        @pl.when(chip >= d)
        def _():
            greet(p - 2 * d, t)
    peers = n_tp
    for d in steps:
        peers = peers + jnp.where(chip + d < chips, 1, 0) + jnp.where(chip >= d, 1, 0)
    pl.semaphore_wait(barrier, peers)

    def raw_copy(k, i, source):
        at = pl.ds(pl.multiple_of(source * seg + i * block, block), block)
        return pltpu.make_async_remote_copy(
            src_ref=tokens.at[pl.ds(i * block, block)],
            dst_ref=raw.at[at],
            send_sem=raw_send.at[k - 1, i],
            recv_sem=raw_recv.at[k - 1, i],
            device_id=(p, lax.rem(t + k, n_tp)),
            device_id_type=MESH,
        )

    for i in range(per_seg):
        for k in range(1, n_tp):
            raw_copy(k, i, t).start()

    row = lax.broadcasted_iota(jnp.int32, (block, block), 0)
    col = lax.broadcasted_iota(jnp.int32, (block, block), 1)
    causal = col <= row
    mid = block // 2 - 1
    sums = jnp.where(
        (col > mid) & (col <= row), 1.0, jnp.where((col <= mid) & (col > row), -1.0, 0.0)
    ).astype(BF16)

    def enter(b):
        rows = pl.ds(pl.multiple_of(b * block, block), block)
        x = raw[rows, :].astype(F32)
        scale = lax.rsqrt(jnp.mean(x * x, axis=1, keepdims=True) + EPS)
        normed = (x * scale * gain[...]).astype(BF16)
        fr = dot(normed, w[1]).astype(BF16).astype(F32)
        values = dot(normed, w[2]).astype(BF16)
        weight = slack[...] / (1.0 + jnp.exp(fr))
        sd = sudden[:, rows]
        sd = jnp.concatenate(
            [
                jnp.transpose(jnp.broadcast_to(sd[h : h + 1, :], (KEY, block)))
                for h in range(heads)
            ],
            axis=1,
        )
        logs = jnp.log1p(-weight) + sd
        high = logs.astype(BF16)
        low = (logs - high.astype(F32)).astype(BF16)
        centred = dot(sums, high) + dot(sums, low)
        ending = centred[block - 1 : block, :]
        to_mid = logs[0:1, :] - centred[0:1, :]
        lifted_k = weight * jnp.exp(-centred)
        kept = (lifted_k * jnp.exp(ending)).astype(BF16)
        lifted_k = lifted_k.astype(BF16)
        mids[b] = jnp.broadcast_to(to_mid, (8, hk))
        cums[b] = jnp.broadcast_to(to_mid + ending, (8, hk))
        for h in range(heads):
            at = slice(h * KEY, (h + 1) * KEY)
            states[b, :, at] = dot(values[:, at], kept[:, at], ((0,), (0,)))
        centres[rows, :] = centred
        keys[rows, :] = lifted_k
        vals[rows, :] = values
        normal[rows, :] = normed

    def leave(b):
        rows = pl.ds(pl.multiple_of(b * block, block), block)
        normed = normal[rows, :]
        centred = centres[rows, :]
        lifted_k = keys[rows, :]
        values = vals[rows, :]
        qr = dot(normed, w[0]).astype(BF16).astype(F32) * KEY ** (-0.5)
        lifted_q = (qr * jnp.exp(centred)).astype(BF16)
        lifted[rows, :] = lifted_q
        gates[rows, :] = dot(normed, w[3]).astype(BF16)
        for h in range(heads):
            at = slice(h * KEY, (h + 1) * KEY)
            scores = dot(lifted_q[:, at], lifted_k[:, at], ((1,), (1,)))
            scores = jnp.where(causal, scores, 0.0).astype(BF16)
            inner[rows, at] = dot(scores, values[:, at])

    own_copy.wait()
    for at, ref in enumerate((wq, wf, wi, wg)):
        pltpu.make_async_copy(ref, w.at[at], w_sem.at[at]).wait()

    def own_block(i, carry):
        enter(t * per_seg + i)
        leave(t * per_seg + i)
        return carry

    lax.fori_loop(0, per_seg, own_block, 0)
    for i in range(per_seg):
        for k in range(1, n_tp):
            source = lax.rem(t + n_tp - k, n_tp)
            raw_copy(k, i, source).wait_recv()
            enter(source * per_seg + i)
            if (i, k) != (per_seg - 1, n_tp - 1):
                leave(source * per_seg + i)

    state = jnp.zeros((KEY, hk), F32)
    total = jnp.zeros((1, hk), F32)
    for b in range(blocks):
        fresh = states[b]
        step_log = cums[b][0:1, :]
        states[b] = state
        cums[b] = jnp.broadcast_to(total, (8, hk))
        state = jnp.exp(step_log) * state + fresh
        total = total + step_log
    decay = jnp.exp(total)

    def fill(ref, s, dec):
        width = dec.shape[1]
        ref[0:KEY, :] = s.astype(BF16)
        hi = dec.astype(BF16).astype(F32)
        lo = dec - hi
        at = lax.broadcasted_iota(jnp.int32, (16, width), 0)
        tail = jnp.where(at == 0, hi, jnp.where(at == 1, lo, 0.0))
        ref[KEY : KEY + 16, :] = tail.astype(BF16)

    def read(ref):
        s = ref[0:KEY, :].astype(F32)
        tail = ref[KEY : KEY + 16, :].astype(F32)
        return s, tail[0:1, :] + tail[1:2, :]

    fill(mine, state, decay)
    pair = pltpu.make_async_remote_copy(
        src_ref=mine, dst_ref=theirs, send_sem=pair_send, recv_sem=pair_recv,
        device_id=(partner, t), device_id_type=MESH,
    )
    pair.start()
    leave(lax.rem(t + 1, n_tp) * per_seg + per_seg - 1)
    pair.wait_recv()
    their_s, their_d = read(theirs)
    first = core == 0
    joined_s = jnp.where(first, their_d * state + their_s, decay * their_s + state)
    joined_d = decay * their_d
    inc_s[...] = jnp.where(first, joined_s[:, :half], joined_s[:, half:])
    inc_d[...] = jnp.broadcast_to(
        jnp.where(first, joined_d[:, :half], joined_d[:, half:]), (8, half)
    )
    exc_s[...] = jnp.zeros_like(exc_s)
    exc_d[...] = jnp.ones_like(exc_d)

    def ks_copy(k, to):
        return pltpu.make_async_remote_copy(
            src_ref=tx.at[k], dst_ref=rx.at[k], send_sem=ks_send.at[k], recv_sem=ks_recv.at[k],
            device_id=(to, t), device_id_type=MESH,
        )

    for k, d in enumerate(steps):
        @pl.when(chip + d < chips)
        def _():
            fill(tx.at[k], inc_s[...], inc_d[0:1, :])
            ks_copy(k, p + 2 * d).start()

        @pl.when(chip >= d)
        def _():
            ks_copy(k, p).wait_recv()
            got_s, got_d = read(rx.at[k])
            exc_s[...] = exc_d[0:1, :] * got_s + exc_s[...]
            exc_d[...] = exc_d[...] * got_d
            if k < len(steps) - 1:
                inc_s[...] = inc_d[0:1, :] * got_s + inc_s[...]
                inc_d[...] = inc_d[...] * got_d

    ex_tx[...] = exc_s[...].astype(BF16)
    swap = pltpu.make_async_remote_copy(
        src_ref=ex_tx, dst_ref=ex_rx, send_sem=ex_send, recv_sem=ex_recv,
        device_id=(partner, t), device_id_type=MESH,
    )
    swap.start()
    swap.wait_recv()
    own_half = exc_s[...]
    other_half = ex_rx[...].astype(F32)
    both = jnp.concatenate(
        [jnp.where(first, own_half, other_half), jnp.where(first, other_half, own_half)], axis=1
    )
    their_s, their_d = read(theirs)
    entry[...] = jnp.where(first, both, their_d * both + their_s)

    def g_copy(k, b, source):
        rows = pl.ds(pl.multiple_of(b * block, block), block)
        return pltpu.make_async_remote_copy(
            src_ref=gated.at[t, rows],
            dst_ref=gated.at[source, rows],
            send_sem=g_send.at[k - 1, b],
            recv_sem=g_recv.at[k - 1, b],
            device_id=(p, lax.rem(t + k, n_tp)),
            device_id_type=MESH,
        )

    def finish(b, carry):
        rows = pl.ds(pl.multiple_of(b * block, block), block)
        at_start = jnp.exp(mids[b][0:1, :]) * (
            states[b] + jnp.exp(cums[b][0:1, :]) * entry[...]
        )
        at_start = at_start.astype(BF16)
        for h in range(heads):
            at = slice(h * KEY, (h + 1) * KEY)
            whole = inner[rows, at] + dot(lifted[rows, at], at_start[:, at], ((1,), (1,)))
            scale = lax.rsqrt(jnp.mean(whole * whole, axis=1, keepdims=True) + EPS)
            g = gates[rows, at].astype(F32)
            result = whole * scale * head_gain[...] * (g / (1.0 + jnp.exp(-g)))
            gated[t, rows, at] = result.astype(BF16)
        for k in range(1, n_tp):
            g_copy(k, b, t).start()
        return carry

    lax.fori_loop(0, blocks, finish, 0)

    def s_copy(k, b, source):
        return pltpu.make_async_remote_copy(
            src_ref=squares.at[t, b],
            dst_ref=squares.at[source, b],
            send_sem=s_send.at[k - 1, b],
            recv_sem=s_recv.at[k - 1, b],
            device_id=(p, lax.rem(t + k, n_tp)),
            device_id_type=MESH,
        )

    pltpu.make_async_copy(wo, ow, w_sem.at[4]).wait()

    def project_own(b, carry):
        rows = pl.ds(pl.multiple_of(b * block, block), block)
        depth = pl.ds(pl.multiple_of(t * hk, hk), hk)
        proj[rows, :] = dot(gated[t, rows, :], ow[depth, :])
        return carry

    lax.fori_loop(0, blocks, project_own, 0)

    def project(b, carry):
        rows = pl.ds(pl.multiple_of(b * block, block), block)
        for k in range(1, n_tp):
            g_copy(k, b, lax.rem(t + n_tp - k, n_tp)).wait_recv()
        acc = proj[rows, :]
        for k in range(1, n_tp):
            source = lax.rem(t + n_tp - k, n_tp)
            depth = pl.ds(pl.multiple_of(source * hk, hk), hk)
            acc = acc + dot(gated[source, rows, :], ow[depth, :])
        proj[rows, :] = acc
        line = jnp.sum(acc * acc, axis=1, keepdims=True)
        square = jnp.transpose(jnp.broadcast_to(line, (block, 128)))
        squares[t, b] = square[0:8, :]
        for k in range(1, n_tp):
            s_copy(k, b, t).start()
        return carry

    lax.fori_loop(0, blocks, project, 0)

    def close(b, carry):
        rows = pl.ds(pl.multiple_of(b * block, block), block)
        for k in range(1, n_tp):
            s_copy(k, b, lax.rem(t + n_tp - k, n_tp)).wait_recv()
        line = squares[0, b][0:1, :]
        for j in range(1, n_tp):
            line = line + squares[j, b][0:1, :]
        column = jnp.transpose(jnp.broadcast_to(line, (128, block)))[:, 0:1]
        out[rows, :] = (
            proj[rows, :] * lax.rsqrt(column * (1.0 / model) + EPS) * out_gain[...]
        ).astype(BF16)
        return carry

    lax.fori_loop(0, blocks, close, 0)

    for i in range(per_seg):
        for k in range(1, n_tp):
            raw_copy(k, i, t).wait_send()
    pair.wait_send()
    for k, d in enumerate(steps):
        @pl.when(chip + d < chips)
        def _():
            ks_copy(k, p + 2 * d).wait_send()
    swap.wait_send()
    for b in range(blocks):
        for k in range(1, n_tp):
            g_copy(k, b, t).wait_send()
            s_copy(k, b, t).wait_send()


def solution(mesh):
    n_sp, n_tp = mesh.shape["sp"], mesh.shape["tp"]

    def shards(tokens, gain, wq, wf, wi, wg, slack, sudden, head_gain, wo, out_gain):
        seg, model = tokens.shape[1:]
        hk = wq.shape[1]
        heads = hk // KEY
        features = wo.shape[1]
        rows_all = seg * n_tp
        block = min(128, seg)
        blocks = rows_all // block
        per_seg = seg // block
        half = hk // 2
        chips = n_sp // 2
        steps = max(1, (chips - 1).bit_length())
        peers = n_tp - 1
        any_spec = pl.BlockSpec(memory_space=pltpu.HBM)
        vmem = pl.BlockSpec(memory_space=pltpu.VMEM)
        dma = pltpu.SemaphoreType.DMA
        cfg = (n_sp, n_tp, seg, block, heads, model)
        call = pl.pallas_call(
            functools.partial(kernel, cfg),
            out_shape=pltpu.VMEM((rows_all, features), BF16),
            in_specs=[
                any_spec, vmem, any_spec, any_spec, any_spec, any_spec,
                vmem, vmem, vmem, any_spec, vmem,
            ],
            out_specs=vmem,
            scratch_shapes=[
                pltpu.VMEM((rows_all, model), BF16),
                pltpu.VMEM((4, model, hk), BF16),
                pltpu.VMEM((hk * n_tp, features), BF16),
                pltpu.VMEM((blocks, KEY, hk), F32),
                pltpu.VMEM((rows_all, hk), F32),
                pltpu.VMEM((rows_all, hk), BF16),
                pltpu.VMEM((rows_all, hk), BF16),
                pltpu.VMEM((blocks, 8, hk), F32),
                pltpu.VMEM((blocks, 8, hk), F32),
                pltpu.VMEM((n_tp, rows_all, hk), BF16),
                pltpu.VMEM((rows_all, features), F32),
                pltpu.VMEM((rows_all, hk), F32),
                pltpu.VMEM((rows_all, hk), BF16),
                pltpu.VMEM((rows_all, hk), BF16),
                pltpu.VMEM((rows_all, model), BF16),
                pltpu.VMEM((KEY + 16, hk), BF16),
                pltpu.VMEM((KEY + 16, hk), BF16),
                pltpu.VMEM((steps, KEY + 16, half), BF16),
                pltpu.VMEM((steps, KEY + 16, half), BF16),
                pltpu.VMEM((KEY, half), F32),
                pltpu.VMEM((8, half), F32),
                pltpu.VMEM((KEY, half), F32),
                pltpu.VMEM((8, half), F32),
                pltpu.VMEM((KEY, half), BF16),
                pltpu.VMEM((KEY, half), BF16),
                pltpu.VMEM((KEY, hk), F32),
                pltpu.VMEM((n_tp, blocks, 8, 128), F32),
                dma((5,)), dma,
                dma((peers, per_seg)), dma((peers, per_seg)),
                dma, dma,
                dma((steps,)), dma((steps,)),
                dma, dma,
                dma((peers, blocks)), dma((peers, blocks)),
                dma((peers, blocks)), dma((peers, blocks)),
            ],
            compiler_params=pltpu.CompilerParams(
                collective_id=0, has_side_effects=True, vmem_limit_bytes=56 * 2**20
            ),
        )
        result = call(
            tokens[0], gain[None], wq, wf, wi, wg, slack[None], sudden[0].T,
            head_gain[None], wo, out_gain[None],
        )
        return result[None]

    placed = (
        P(None, ("sp", "tp"), None),
        P(),
        P(None, "tp"),
        P(None, "tp"),
        P(None, "tp"),
        P(None, "tp"),
        P("tp"),
        P(None, "sp", "tp"),
        P(),
        P(None, "tp"),
        P("tp"),
    )
    return jax.shard_map(
        shards, mesh=mesh, in_specs=placed, out_specs=P(None, "sp", "tp"), check_vma=False
    )
```

```python
import functools

import jax
import jax.numpy as jnp
from jax import lax
from jax.experimental import pallas as pl
from jax.experimental.pallas import tpu as pltpu
from jax.sharding import PartitionSpec as P

KEY = 128
EPS = 1e-06
MESH = pl.DeviceIdType.MESH
F32 = jnp.float32
BF16 = jnp.bfloat16


def dot(a, b, dims=((1,), (0,))):
    return lax.dot_general(a, b, (dims, ((), ())), preferred_element_type=F32)


def kernel(
    cfg,
    tokens, gain, wq, wf, wi, wg, slack, sudden, head_gain, wo, out_gain,
    out,
    raw, w, ow, states, inner, lifted, gates, mids, cums, gated, proj, centres, keys, vals, normal,
    mine, theirs, tx, rx, inc_s, inc_d, exc_s, exc_d, ex_tx, ex_rx, entry,
    squares,
    w_sem, ow_sem, own_sem, raw_send, raw_recv, pair_send, pair_recv, ks_send, ks_recv,
    ex_send, ex_recv, g_send, g_recv, s_send, s_recv,
):
    n_sp, n_tp, seg, block, heads, model = cfg
    rows_all = seg * n_tp
    blocks = rows_all // block
    per_seg = seg // block
    hk = heads * KEY
    half = hk // 2
    chips = n_sp // 2
    steps = []
    d = 1
    while d < chips:
        steps.append(d)
        d *= 2
    p = lax.axis_index("sp")
    t = lax.axis_index("tp")
    core = lax.rem(p, 2)
    chip = p // 2
    partner = p + 1 - 2 * core

    for at, ref in enumerate((wq, wf, wi, wg)):
        pltpu.make_async_copy(ref, w.at[at], w_sem.at[at]).start()
    own_rows = pl.ds(pl.multiple_of(t * seg, seg), seg)
    own_copy = pltpu.make_async_copy(tokens, raw.at[own_rows], own_sem)
    own_copy.start()
    groups = half // KEY

    def ow_copies():
        for j in range(n_tp):
            for h in range(heads):
                place = j * heads + (h % groups) * 2 + h // groups
                yield pltpu.make_async_copy(
                    wo.at[pl.ds((j * heads + h) * KEY, KEY)],
                    ow.at[pl.ds(place * KEY, KEY)],
                    ow_sem.at[j * heads + h],
                )

    for copy in ow_copies():
        copy.start()

    barrier = pltpu.get_barrier_semaphore()

    def greet(sp_at, tp_at):
        pl.semaphore_signal(barrier, inc=1, device_id=(sp_at, tp_at), device_id_type=MESH)

    for k in range(1, n_tp):
        greet(p, lax.rem(t + k, n_tp))
    greet(partner, t)
    for d in steps:
        @pl.when(chip + d < chips)
        def _():
            greet(p + 2 * d, t)

        @pl.when(chip >= d)
        def _():
            greet(p - 2 * d, t)
    peers = n_tp
    for d in steps:
        peers = peers + jnp.where(chip + d < chips, 1, 0) + jnp.where(chip >= d, 1, 0)
    pl.semaphore_wait(barrier, peers)

    def raw_copy(k, i, source):
        at = pl.ds(pl.multiple_of(source * seg + i * block, block), block)
        return pltpu.make_async_remote_copy(
            src_ref=tokens.at[pl.ds(i * block, block)],
            dst_ref=raw.at[at],
            send_sem=raw_send.at[k - 1, i],
            recv_sem=raw_recv.at[k - 1, i],
            device_id=(p, lax.rem(t + k, n_tp)),
            device_id_type=MESH,
        )

    for i in range(per_seg):
        for k in range(1, n_tp):
            raw_copy(k, i, t).start()

    row = lax.broadcasted_iota(jnp.int32, (block, block), 0)
    col = lax.broadcasted_iota(jnp.int32, (block, block), 1)
    causal = col <= row
    mid = block // 2 - 1
    sums = jnp.where(
        (col > mid) & (col <= row), 1.0, jnp.where((col <= mid) & (col > row), -1.0, 0.0)
    ).astype(BF16)

    def enter(b):
        rows = pl.ds(pl.multiple_of(b * block, block), block)
        x = raw[rows, :].astype(F32)
        scale = lax.rsqrt(jnp.mean(x * x, axis=1, keepdims=True) + EPS)
        normed = (x * scale * gain[...]).astype(BF16)
        fr = dot(normed, w[1]).astype(BF16).astype(F32)
        values = dot(normed, w[2]).astype(BF16)
        weight = slack[...] / (1.0 + jnp.exp(fr))
        sd = sudden[:, rows]
        sd = jnp.concatenate(
            [
                jnp.transpose(jnp.broadcast_to(sd[h : h + 1, :], (KEY, block)))
                for h in range(heads)
            ],
            axis=1,
        )
        logs = jnp.log1p(-weight) + sd
        high = logs.astype(BF16)
        low = (logs - high.astype(F32)).astype(BF16)
        centred = dot(sums, high) + dot(sums, low)
        ending = centred[block - 1 : block, :]
        to_mid = logs[0:1, :] - centred[0:1, :]
        lifted_k = weight * jnp.exp(-centred)
        kept = (lifted_k * jnp.exp(ending)).astype(BF16)
        lifted_k = lifted_k.astype(BF16)
        mids[b] = jnp.broadcast_to(to_mid, (8, hk))
        cums[b] = jnp.broadcast_to(to_mid + ending, (8, hk))
        for h in range(heads):
            at = slice(h * KEY, (h + 1) * KEY)
            states[b, :, at] = dot(values[:, at], kept[:, at], ((0,), (0,)))
        centres[rows, :] = centred
        keys[rows, :] = lifted_k
        vals[rows, :] = values
        normal[rows, :] = normed

    def leave(b):
        rows = pl.ds(pl.multiple_of(b * block, block), block)
        normed = normal[rows, :]
        centred = centres[rows, :]
        lifted_k = keys[rows, :]
        values = vals[rows, :]
        qr = dot(normed, w[0]).astype(BF16).astype(F32) * KEY ** (-0.5)
        lifted_q = (qr * jnp.exp(centred)).astype(BF16)
        lifted[rows, :] = lifted_q
        g = dot(normed, w[3]).astype(BF16).astype(F32)
        wide_gain = jnp.concatenate([head_gain[...]] * heads, axis=1)
        gates[rows, :] = wide_gain * (g / (1.0 + jnp.exp(-g)))
        for h in range(heads):
            at = slice(h * KEY, (h + 1) * KEY)
            scores = dot(lifted_q[:, at], lifted_k[:, at], ((1,), (1,)))
            scores = jnp.where(causal, scores, 0.0).astype(BF16)
            inner[rows, at] = dot(scores, values[:, at])

    own_copy.wait()
    for at, ref in enumerate((wq, wf, wi, wg)):
        pltpu.make_async_copy(ref, w.at[at], w_sem.at[at]).wait()

    def own_block(i, carry):
        enter(t * per_seg + i)
        leave(t * per_seg + i)
        return carry

    lax.fori_loop(0, per_seg, own_block, 0)
    for i in range(per_seg):
        for k in range(1, n_tp):
            source = lax.rem(t + n_tp - k, n_tp)
            raw_copy(k, i, source).wait_recv()
            enter(source * per_seg + i)
            if (i, k) != (per_seg - 1, n_tp - 1):
                leave(source * per_seg + i)

    state = jnp.zeros((KEY, hk), F32)
    total = jnp.zeros((1, hk), F32)
    for b in range(blocks):
        fresh = states[b]
        step_log = cums[b][0:1, :]
        states[b] = state
        cums[b] = jnp.broadcast_to(total, (8, hk))
        state = jnp.exp(step_log) * state + fresh
        total = total + step_log
    decay = jnp.exp(total)

    def fill(ref, s, dec):
        width = dec.shape[1]
        ref[0:KEY, :] = s.astype(BF16)
        hi = dec.astype(BF16).astype(F32)
        lo = dec - hi
        at = lax.broadcasted_iota(jnp.int32, (16, width), 0)
        tail = jnp.where(at == 0, hi, jnp.where(at == 1, lo, 0.0))
        ref[KEY : KEY + 16, :] = tail.astype(BF16)

    def read(ref):
        s = ref[0:KEY, :].astype(F32)
        tail = ref[KEY : KEY + 16, :].astype(F32)
        return s, tail[0:1, :] + tail[1:2, :]

    fill(mine, state, decay)
    pair = pltpu.make_async_remote_copy(
        src_ref=mine, dst_ref=theirs, send_sem=pair_send, recv_sem=pair_recv,
        device_id=(partner, t), device_id_type=MESH,
    )
    pair.start()
    leave(lax.rem(t + 1, n_tp) * per_seg + per_seg - 1)
    pair.wait_recv()
    their_s, their_d = read(theirs)
    first = core == 0
    joined_s = jnp.where(first, their_d * state + their_s, decay * their_s + state)
    joined_d = decay * their_d
    for g in range(groups):
        near = slice(g * KEY, (g + 1) * KEY)
        far = slice(half + g * KEY, half + (g + 1) * KEY)
        inc_s[g] = jnp.where(first, joined_s[:, near], joined_s[:, far])
        inc_d[g] = jnp.broadcast_to(
            jnp.where(first, joined_d[:, near], joined_d[:, far]), (8, KEY)
        )
    exc_s[...] = jnp.zeros_like(exc_s)
    exc_d[...] = jnp.ones_like(exc_d)

    def ks_copy(k, g, to):
        return pltpu.make_async_remote_copy(
            src_ref=tx.at[k, g], dst_ref=rx.at[k, g],
            send_sem=ks_send.at[k, g], recv_sem=ks_recv.at[k, g],
            device_id=(to, t), device_id_type=MESH,
        )

    def ks_start(k, g):
        @pl.when(chip + steps[k] < chips)
        def _():
            fill(tx.at[k, g], inc_s[g], inc_d[g][0:1, :])
            ks_copy(k, g, p + 2 * steps[k]).start()

    def ks_take(k, g):
        @pl.when(chip >= steps[k])
        def _():
            ks_copy(k, g, p).wait_recv()
            got_s, got_d = read(rx.at[k, g])
            exc_s[g] = exc_d[g][0:1, :] * got_s + exc_s[g]
            exc_d[g] = exc_d[g] * got_d
            if k < len(steps) - 1:
                inc_s[g] = inc_d[g][0:1, :] * got_s + inc_s[g]
                inc_d[g] = inc_d[g] * got_d

    def swap_copy(g):
        return pltpu.make_async_remote_copy(
            src_ref=ex_tx.at[g], dst_ref=ex_rx.at[g],
            send_sem=ex_send.at[g], recv_sem=ex_recv.at[g],
            device_id=(partner, t), device_id_type=MESH,
        )

    def g_copy(k, g, b, source):
        rows = pl.ds(pl.multiple_of(b * block, block), block)
        return pltpu.make_async_remote_copy(
            src_ref=gated.at[t, g, rows],
            dst_ref=gated.at[source, g, rows],
            send_sem=g_send.at[k - 1, g, b],
            recv_sem=g_recv.at[k - 1, g, b],
            device_id=(p, lax.rem(t + k, n_tp)),
            device_id_type=MESH,
        )

    if steps:
        for g in range(groups):
            ks_start(0, g)
    for k in range(len(steps) - 1):
        for g in range(groups):
            ks_take(k, g)
            ks_start(k + 1, g)
    for g in range(groups):
        if steps:
            ks_take(len(steps) - 1, g)
        ex_tx[g] = exc_s[g].astype(BF16)
        swap_copy(g).start()
        swap_copy(g).wait_recv()
        own_part = exc_s[g]
        other_part = ex_rx[g].astype(F32)
        pieces = (
            jnp.where(first, own_part, other_part), jnp.where(first, other_part, own_part)
        )
        for c, piece in enumerate(pieces):
            h = c * groups + g
            at = slice(h * KEY, (h + 1) * KEY)
            past_s = theirs[0:KEY, at].astype(F32)
            tail = theirs[KEY : KEY + 16, at].astype(F32)
            past_d = tail[0:1, :] + tail[1:2, :]
            entry[:, c * KEY : (c + 1) * KEY] = jnp.where(
                first, piece, past_d * piece + past_s
            )

        def finish(b, carry):
            rows = pl.ds(pl.multiple_of(b * block, block), block)
            for c in range(2):
                h = c * groups + g
                at = slice(h * KEY, (h + 1) * KEY)
                side = slice(c * KEY, (c + 1) * KEY)
                at_start = jnp.exp(mids[b, 0:1, at]) * (
                    states[b, :, at] + jnp.exp(cums[b, 0:1, at]) * entry[:, side]
                )
                whole = inner[rows, at] + dot(
                    lifted[rows, at], at_start.astype(BF16), ((1,), (1,))
                )
                scale = lax.rsqrt(jnp.mean(whole * whole, axis=1, keepdims=True) + EPS)
                gated[t, g, rows, side] = (whole * scale * gates[rows, at]).astype(BF16)
            for k in range(1, n_tp):
                g_copy(k, g, b, t).start()
            return carry

        lax.fori_loop(0, blocks, finish, 0)

    def s_copy(k, b, source):
        return pltpu.make_async_remote_copy(
            src_ref=squares.at[t, b],
            dst_ref=squares.at[source, b],
            send_sem=s_send.at[k - 1, b],
            recv_sem=s_recv.at[k - 1, b],
            device_id=(p, lax.rem(t + k, n_tp)),
            device_id_type=MESH,
        )

    for copy in ow_copies():
        copy.wait()

    def depth_of(j, g):
        return pl.ds(pl.multiple_of(j * hk + g * 2 * KEY, 2 * KEY), 2 * KEY)

    def project_own(b, carry):
        rows = pl.ds(pl.multiple_of(b * block, block), block)
        acc = dot(gated[t, 0, rows, :], ow[depth_of(t, 0), :])
        for g in range(1, groups):
            acc = acc + dot(gated[t, g, rows, :], ow[depth_of(t, g), :])
        proj[rows, :] = acc
        return carry

    lax.fori_loop(0, blocks, project_own, 0)

    def peers_part(b, g):
        rows = pl.ds(pl.multiple_of(b * block, block), block)
        acc = proj[rows, :]
        for k in range(1, n_tp):
            source = lax.rem(t + n_tp - k, n_tp)
            g_copy(k, g, b, source).wait_recv()
            acc = acc + dot(gated[source, g, rows, :], ow[depth_of(source, g), :])
        return acc

    for g in range(groups - 1):
        def project_early(b, carry):
            rows = pl.ds(pl.multiple_of(b * block, block), block)
            proj[rows, :] = peers_part(b, g)
            return carry

        lax.fori_loop(0, blocks, project_early, 0)

    def project(b, carry):
        rows = pl.ds(pl.multiple_of(b * block, block), block)
        acc = peers_part(b, groups - 1)
        proj[rows, :] = acc
        line = jnp.sum(acc * acc, axis=1, keepdims=True)
        square = jnp.transpose(jnp.broadcast_to(line, (block, 128)))
        squares[t, b] = square[0:8, :]
        for k in range(1, n_tp):
            s_copy(k, b, t).start()
        return carry

    lax.fori_loop(0, blocks, project, 0)

    def close(b, carry):
        rows = pl.ds(pl.multiple_of(b * block, block), block)
        for k in range(1, n_tp):
            s_copy(k, b, lax.rem(t + n_tp - k, n_tp)).wait_recv()
        line = squares[0, b][0:1, :]
        for j in range(1, n_tp):
            line = line + squares[j, b][0:1, :]
        column = jnp.transpose(jnp.broadcast_to(line, (128, block)))[:, 0:1]
        out[rows, :] = (
            proj[rows, :] * lax.rsqrt(column * (1.0 / model) + EPS) * out_gain[...]
        ).astype(BF16)
        return carry

    lax.fori_loop(0, blocks, close, 0)

    for i in range(per_seg):
        for k in range(1, n_tp):
            raw_copy(k, i, t).wait_send()
    pair.wait_send()
    for k, d in enumerate(steps):
        @pl.when(chip + d < chips)
        def _():
            for g in range(groups):
                ks_copy(k, g, p + 2 * d).wait_send()
    for g in range(groups):
        swap_copy(g).wait_send()
    for b in range(blocks):
        for k in range(1, n_tp):
            for g in range(groups):
                g_copy(k, g, b, t).wait_send()
            s_copy(k, b, t).wait_send()


def solution(mesh):
    n_sp, n_tp = mesh.shape["sp"], mesh.shape["tp"]

    def shards(tokens, gain, wq, wf, wi, wg, slack, sudden, head_gain, wo, out_gain):
        seg, model = tokens.shape[1:]
        hk = wq.shape[1]
        heads = hk // KEY
        features = wo.shape[1]
        rows_all = seg * n_tp
        block = min(128, seg)
        blocks = rows_all // block
        per_seg = seg // block
        groups = hk // 2 // KEY
        chips = n_sp // 2
        steps = max(1, (chips - 1).bit_length())
        peers = n_tp - 1
        any_spec = pl.BlockSpec(memory_space=pltpu.HBM)
        vmem = pl.BlockSpec(memory_space=pltpu.VMEM)
        dma = pltpu.SemaphoreType.DMA
        cfg = (n_sp, n_tp, seg, block, heads, model)
        call = pl.pallas_call(
            functools.partial(kernel, cfg),
            out_shape=pltpu.VMEM((rows_all, features), BF16),
            in_specs=[
                any_spec, vmem, any_spec, any_spec, any_spec, any_spec,
                vmem, vmem, vmem, any_spec, vmem,
            ],
            out_specs=vmem,
            scratch_shapes=[
                pltpu.VMEM((rows_all, model), BF16),
                pltpu.VMEM((4, model, hk), BF16),
                pltpu.VMEM((hk * n_tp, features), BF16),
                pltpu.VMEM((blocks, KEY, hk), F32),
                pltpu.VMEM((rows_all, hk), F32),
                pltpu.VMEM((rows_all, hk), BF16),
                pltpu.VMEM((rows_all, hk), F32),
                pltpu.VMEM((blocks, 8, hk), F32),
                pltpu.VMEM((blocks, 8, hk), F32),
                pltpu.VMEM((n_tp, groups, rows_all, 2 * KEY), BF16),
                pltpu.VMEM((rows_all, features), F32),
                pltpu.VMEM((rows_all, hk), F32),
                pltpu.VMEM((rows_all, hk), BF16),
                pltpu.VMEM((rows_all, hk), BF16),
                pltpu.VMEM((rows_all, model), BF16),
                pltpu.VMEM((KEY + 16, hk), BF16),
                pltpu.VMEM((KEY + 16, hk), BF16),
                pltpu.VMEM((steps, groups, KEY + 16, KEY), BF16),
                pltpu.VMEM((steps, groups, KEY + 16, KEY), BF16),
                pltpu.VMEM((groups, KEY, KEY), F32),
                pltpu.VMEM((groups, 8, KEY), F32),
                pltpu.VMEM((groups, KEY, KEY), F32),
                pltpu.VMEM((groups, 8, KEY), F32),
                pltpu.VMEM((groups, KEY, KEY), BF16),
                pltpu.VMEM((groups, KEY, KEY), BF16),
                pltpu.VMEM((KEY, 2 * KEY), F32),
                pltpu.VMEM((n_tp, blocks, 8, 128), F32),
                dma((4,)), dma((heads * n_tp,)), dma,
                dma((peers, per_seg)), dma((peers, per_seg)),
                dma, dma,
                dma((steps, groups)), dma((steps, groups)),
                dma((groups,)), dma((groups,)),
                dma((peers, groups, blocks)), dma((peers, groups, blocks)),
                dma((peers, blocks)), dma((peers, blocks)),
            ],
            compiler_params=pltpu.CompilerParams(
                collective_id=0, has_side_effects=True, vmem_limit_bytes=56 * 2**20
            ),
        )
        result = call(
            tokens[0], gain[None], wq, wf, wi, wg, slack[None], sudden[0].T,
            head_gain[None], wo, out_gain[None],
        )
        return result[None]

    placed = (
        P(None, ("sp", "tp"), None),
        P(),
        P(None, "tp"),
        P(None, "tp"),
        P(None, "tp"),
        P(None, "tp"),
        P("tp"),
        P(None, "sp", "tp"),
        P(),
        P(None, "tp"),
        P("tp"),
    )
    return jax.shard_map(
        shards, mesh=mesh, in_specs=placed, out_specs=P(None, "sp", "tp"), check_vma=False
    )
```

```python
import functools

import jax
import jax.numpy as jnp
from jax import lax
from jax.experimental import pallas as pl
from jax.experimental.pallas import tpu as pltpu
from jax.sharding import PartitionSpec as P

KEY = 128
EPS = 1e-06
MESH = pl.DeviceIdType.MESH
F32 = jnp.float32
BF16 = jnp.bfloat16


def dot(a, b, dims=((1,), (0,))):
    return lax.dot_general(a, b, (dims, ((), ())), preferred_element_type=F32)


def kernel(
    cfg,
    tokens, gain, wq, wf, wi, wg, slack, sudden, head_gain, wo, out_gain,
    out,
    raw, w, ow, states, inner, lifted, gates, mids, cums, gated, proj, centres, keys, vals, normal,
    mine, theirs, tx, rx, inc_s, inc_d, exc_s, exc_d, ex_tx, ex_rx, entry,
    squares,
    w_sem, ow_sem, own_sem, raw_send, raw_recv, pair_send, pair_recv, ks_send, ks_recv,
    ex_send, ex_recv, g_send, g_recv, s_send, s_recv,
):
    n_sp, n_tp, seg, block, heads, model = cfg
    rows_all = seg * n_tp
    blocks = rows_all // block
    per_seg = seg // block
    hk = heads * KEY
    half = hk // 2
    chips = n_sp // 2
    steps = []
    d = 1
    while d < chips:
        steps.append(d)
        d *= 2
    p = lax.axis_index("sp")
    t = lax.axis_index("tp")
    core = lax.rem(p, 2)
    chip = p // 2
    partner = p + 1 - 2 * core

    for at, ref in enumerate((wq, wf, wi, wg)):
        pltpu.make_async_copy(ref, w.at[at], w_sem.at[at]).start()
    own_rows = pl.ds(pl.multiple_of(t * seg, seg), seg)
    own_copy = pltpu.make_async_copy(tokens, raw.at[own_rows], own_sem)
    own_copy.start()
    groups = half // KEY

    def ow_copies():
        for j in range(n_tp):
            for h in range(heads):
                place = j * heads + (h % groups) * 2 + h // groups
                yield pltpu.make_async_copy(
                    wo.at[pl.ds((j * heads + h) * KEY, KEY)],
                    ow.at[pl.ds(place * KEY, KEY)],
                    ow_sem.at[j * heads + h],
                )

    for copy in ow_copies():
        copy.start()

    barrier = pltpu.get_barrier_semaphore()

    def greet(sp_at, tp_at):
        pl.semaphore_signal(barrier, inc=1, device_id=(sp_at, tp_at), device_id_type=MESH)

    for k in range(1, n_tp):
        greet(p, lax.rem(t + k, n_tp))
    greet(partner, t)
    for d in steps:
        @pl.when(chip + d < chips)
        def _():
            greet(p + 2 * d, t)

        @pl.when(chip >= d)
        def _():
            greet(p - 2 * d, t)
    peers = n_tp
    for d in steps:
        peers = peers + jnp.where(chip + d < chips, 1, 0) + jnp.where(chip >= d, 1, 0)
    pl.semaphore_wait(barrier, peers)

    def raw_copy(k, i, source):
        at = pl.ds(pl.multiple_of(source * seg + i * block, block), block)
        return pltpu.make_async_remote_copy(
            src_ref=tokens.at[pl.ds(i * block, block)],
            dst_ref=raw.at[at],
            send_sem=raw_send.at[k - 1, i],
            recv_sem=raw_recv.at[k - 1, i],
            device_id=(p, lax.rem(t + k, n_tp)),
            device_id_type=MESH,
        )

    for i in range(per_seg):
        for k in range(1, n_tp):
            raw_copy(k, i, t).start()

    row = lax.broadcasted_iota(jnp.int32, (block, block), 0)
    col = lax.broadcasted_iota(jnp.int32, (block, block), 1)
    causal = col <= row
    mid = block // 2 - 1
    sums = jnp.where(
        (col > mid) & (col <= row), 1.0, jnp.where((col <= mid) & (col > row), -1.0, 0.0)
    ).astype(BF16)

    def enter(b):
        rows = pl.ds(pl.multiple_of(b * block, block), block)
        x = raw[rows, :].astype(F32)
        scale = lax.rsqrt(jnp.mean(x * x, axis=1, keepdims=True) + EPS)
        normed = (x * scale * gain[...]).astype(BF16)
        fr = dot(normed, w[1]).astype(BF16).astype(F32)
        values = dot(normed, w[2]).astype(BF16)
        weight = slack[...] / (1.0 + jnp.exp(fr))
        sd = sudden[:, rows]
        sd = jnp.concatenate(
            [
                jnp.transpose(jnp.broadcast_to(sd[h : h + 1, :], (KEY, block)))
                for h in range(heads)
            ],
            axis=1,
        )
        logs = jnp.log1p(-weight) + sd
        high = logs.astype(BF16)
        low = (logs - high.astype(F32)).astype(BF16)
        centred = dot(sums, high) + dot(sums, low)
        ending = centred[block - 1 : block, :]
        to_mid = logs[0:1, :] - centred[0:1, :]
        lifted_k = weight * jnp.exp(-centred)
        kept = (lifted_k * jnp.exp(ending)).astype(BF16)
        lifted_k = lifted_k.astype(BF16)
        mids[b] = jnp.broadcast_to(to_mid, (8, hk))
        cums[b] = jnp.broadcast_to(to_mid + ending, (8, hk))
        for h in range(heads):
            at = slice(h * KEY, (h + 1) * KEY)
            states[b, :, at] = dot(values[:, at], kept[:, at], ((0,), (0,)))
        centres[rows, :] = centred
        keys[rows, :] = lifted_k
        vals[rows, :] = values
        normal[rows, :] = normed

    def leave(b):
        rows = pl.ds(pl.multiple_of(b * block, block), block)
        normed = normal[rows, :]
        centred = centres[rows, :]
        lifted_k = keys[rows, :]
        values = vals[rows, :]
        qr = dot(normed, w[0]).astype(BF16).astype(F32) * KEY ** (-0.5)
        lifted_q = (qr * jnp.exp(centred)).astype(BF16)
        lifted[rows, :] = lifted_q
        g = dot(normed, w[3]).astype(BF16).astype(F32)
        wide_gain = jnp.concatenate([head_gain[...]] * heads, axis=1)
        gates[rows, :] = wide_gain * (g / (1.0 + jnp.exp(-g)))
        for h in range(heads):
            at = slice(h * KEY, (h + 1) * KEY)
            scores = dot(lifted_q[:, at], lifted_k[:, at], ((1,), (1,)))
            scores = jnp.where(causal, scores, 0.0).astype(BF16)
            inner[rows, at] = dot(scores, values[:, at])

    own_copy.wait()
    for at, ref in enumerate((wq, wf, wi, wg)):
        pltpu.make_async_copy(ref, w.at[at], w_sem.at[at]).wait()

    def own_block(i, carry):
        enter(t * per_seg + i)
        leave(t * per_seg + i)
        return carry

    lax.fori_loop(0, per_seg, own_block, 0)
    for i in range(per_seg):
        for k in range(1, n_tp):
            source = lax.rem(t + n_tp - k, n_tp)
            raw_copy(k, i, source).wait_recv()
            enter(source * per_seg + i)
            if (i, k) != (per_seg - 1, n_tp - 1):
                leave(source * per_seg + i)

    state = jnp.zeros((KEY, hk), F32)
    total = jnp.zeros((1, hk), F32)
    for b in range(blocks):
        fresh = states[b]
        step_log = cums[b][0:1, :]
        states[b] = state
        cums[b] = jnp.broadcast_to(total, (8, hk))
        state = jnp.exp(step_log) * state + fresh
        total = total + step_log
    decay = jnp.exp(total)

    def fill(ref, s, dec):
        width = dec.shape[1]
        ref[0:KEY, :] = s.astype(BF16)
        hi = dec.astype(BF16).astype(F32)
        lo = dec - hi
        at = lax.broadcasted_iota(jnp.int32, (16, width), 0)
        tail = jnp.where(at == 0, hi, jnp.where(at == 1, lo, 0.0))
        ref[KEY : KEY + 16, :] = tail.astype(BF16)

    def read(ref):
        s = ref[0:KEY, :].astype(F32)
        tail = ref[KEY : KEY + 16, :].astype(F32)
        return s, tail[0:1, :] + tail[1:2, :]

    fill(mine, state, decay)
    pair = pltpu.make_async_remote_copy(
        src_ref=mine, dst_ref=theirs, send_sem=pair_send, recv_sem=pair_recv,
        device_id=(partner, t), device_id_type=MESH,
    )
    pair.start()
    pair.wait_recv()
    their_s, their_d = read(theirs)
    first = core == 0
    joined_s = jnp.where(first, their_d * state + their_s, decay * their_s + state)
    joined_d = decay * their_d
    for g in range(groups):
        near = slice(g * KEY, (g + 1) * KEY)
        far = slice(half + g * KEY, half + (g + 1) * KEY)
        inc_s[g] = jnp.where(first, joined_s[:, near], joined_s[:, far])
        inc_d[g] = jnp.broadcast_to(
            jnp.where(first, joined_d[:, near], joined_d[:, far]), (8, KEY)
        )
    exc_s[...] = jnp.zeros_like(exc_s)
    exc_d[...] = jnp.ones_like(exc_d)

    def ks_copy(k, g, to):
        return pltpu.make_async_remote_copy(
            src_ref=tx.at[k, g], dst_ref=rx.at[k, g],
            send_sem=ks_send.at[k, g], recv_sem=ks_recv.at[k, g],
            device_id=(to, t), device_id_type=MESH,
        )

    def ks_start(k, g):
        @pl.when(chip + steps[k] < chips)
        def _():
            fill(tx.at[k, g], inc_s[g], inc_d[g][0:1, :])
            ks_copy(k, g, p + 2 * steps[k]).start()

    def ks_take(k, g):
        @pl.when(chip >= steps[k])
        def _():
            ks_copy(k, g, p).wait_recv()
            got_s, got_d = read(rx.at[k, g])
            exc_s[g] = exc_d[g][0:1, :] * got_s + exc_s[g]
            exc_d[g] = exc_d[g] * got_d
            if k < len(steps) - 1:
                inc_s[g] = inc_d[g][0:1, :] * got_s + inc_s[g]
                inc_d[g] = inc_d[g] * got_d

    def swap_copy(g):
        return pltpu.make_async_remote_copy(
            src_ref=ex_tx.at[g], dst_ref=ex_rx.at[g],
            send_sem=ex_send.at[g], recv_sem=ex_recv.at[g],
            device_id=(partner, t), device_id_type=MESH,
        )

    def g_copy(k, g, b, source):
        rows = pl.ds(pl.multiple_of(b * block, block), block)
        return pltpu.make_async_remote_copy(
            src_ref=gated.at[t, g, rows],
            dst_ref=gated.at[source, g, rows],
            send_sem=g_send.at[k - 1, g, b],
            recv_sem=g_recv.at[k - 1, g, b],
            device_id=(p, lax.rem(t + k, n_tp)),
            device_id_type=MESH,
        )

    if steps:
        for g in range(groups):
            ks_start(0, g)
    leave(lax.rem(t + 1, n_tp) * per_seg + per_seg - 1)
    for k in range(len(steps) - 1):
        for g in range(groups):
            ks_take(k, g)
            ks_start(k + 1, g)
    for g in range(groups):
        if steps:
            ks_take(len(steps) - 1, g)
        ex_tx[g] = exc_s[g].astype(BF16)
        swap_copy(g).start()
        swap_copy(g).wait_recv()
        own_part = exc_s[g]
        other_part = ex_rx[g].astype(F32)
        pieces = (
            jnp.where(first, own_part, other_part), jnp.where(first, other_part, own_part)
        )
        for c, piece in enumerate(pieces):
            h = c * groups + g
            at = slice(h * KEY, (h + 1) * KEY)
            past_s = theirs[0:KEY, at].astype(F32)
            tail = theirs[KEY : KEY + 16, at].astype(F32)
            past_d = tail[0:1, :] + tail[1:2, :]
            entry[:, c * KEY : (c + 1) * KEY] = jnp.where(
                first, piece, past_d * piece + past_s
            )

        def finish(b, carry):
            rows = pl.ds(pl.multiple_of(b * block, block), block)
            for c in range(2):
                h = c * groups + g
                at = slice(h * KEY, (h + 1) * KEY)
                side = slice(c * KEY, (c + 1) * KEY)
                at_start = jnp.exp(mids[b, 0:1, at]) * (
                    states[b, :, at] + jnp.exp(cums[b, 0:1, at]) * entry[:, side]
                )
                whole = inner[rows, at] + dot(
                    lifted[rows, at], at_start.astype(BF16), ((1,), (1,))
                )
                scale = lax.rsqrt(jnp.mean(whole * whole, axis=1, keepdims=True) + EPS)
                gated[t, g, rows, side] = (whole * scale * gates[rows, at]).astype(BF16)
            for k in range(1, n_tp):
                g_copy(k, g, b, t).start()
            return carry

        lax.fori_loop(0, blocks, finish, 0)

    def s_copy(k, b, source):
        return pltpu.make_async_remote_copy(
            src_ref=squares.at[t, b],
            dst_ref=squares.at[source, b],
            send_sem=s_send.at[k - 1, b],
            recv_sem=s_recv.at[k - 1, b],
            device_id=(p, lax.rem(t + k, n_tp)),
            device_id_type=MESH,
        )

    for copy in ow_copies():
        copy.wait()

    def depth_of(j, g):
        return pl.ds(pl.multiple_of(j * hk + g * 2 * KEY, 2 * KEY), 2 * KEY)

    def project_own(b, carry):
        rows = pl.ds(pl.multiple_of(b * block, block), block)
        acc = dot(gated[t, 0, rows, :], ow[depth_of(t, 0), :])
        for g in range(1, groups):
            acc = acc + dot(gated[t, g, rows, :], ow[depth_of(t, g), :])
        proj[rows, :] = acc
        return carry

    lax.fori_loop(0, blocks, project_own, 0)

    def peers_part(b, g):
        rows = pl.ds(pl.multiple_of(b * block, block), block)
        acc = proj[rows, :]
        for k in range(1, n_tp):
            source = lax.rem(t + n_tp - k, n_tp)
            g_copy(k, g, b, source).wait_recv()
            acc = acc + dot(gated[source, g, rows, :], ow[depth_of(source, g), :])
        return acc

    for g in range(groups - 1):
        def project_early(b, carry):
            rows = pl.ds(pl.multiple_of(b * block, block), block)
            proj[rows, :] = peers_part(b, g)
            return carry

        lax.fori_loop(0, blocks, project_early, 0)

    def project(b, carry):
        rows = pl.ds(pl.multiple_of(b * block, block), block)
        acc = peers_part(b, groups - 1)
        proj[rows, :] = acc
        line = jnp.sum(acc * acc, axis=1, keepdims=True)
        square = jnp.transpose(jnp.broadcast_to(line, (block, 128)))
        squares[t, b] = square[0:8, :]
        for k in range(1, n_tp):
            s_copy(k, b, t).start()
        return carry

    lax.fori_loop(0, blocks, project, 0)

    def close(b, carry):
        rows = pl.ds(pl.multiple_of(b * block, block), block)
        for k in range(1, n_tp):
            s_copy(k, b, lax.rem(t + n_tp - k, n_tp)).wait_recv()
        line = squares[0, b][0:1, :]
        for j in range(1, n_tp):
            line = line + squares[j, b][0:1, :]
        column = jnp.transpose(jnp.broadcast_to(line, (128, block)))[:, 0:1]
        out[rows, :] = (
            proj[rows, :] * lax.rsqrt(column * (1.0 / model) + EPS) * out_gain[...]
        ).astype(BF16)
        return carry

    lax.fori_loop(0, blocks, close, 0)

    for i in range(per_seg):
        for k in range(1, n_tp):
            raw_copy(k, i, t).wait_send()
    pair.wait_send()
    for k, d in enumerate(steps):
        @pl.when(chip + d < chips)
        def _():
            for g in range(groups):
                ks_copy(k, g, p + 2 * d).wait_send()
    for g in range(groups):
        swap_copy(g).wait_send()
    for b in range(blocks):
        for k in range(1, n_tp):
            for g in range(groups):
                g_copy(k, g, b, t).wait_send()
            s_copy(k, b, t).wait_send()


def solution(mesh):
    n_sp, n_tp = mesh.shape["sp"], mesh.shape["tp"]

    def shards(tokens, gain, wq, wf, wi, wg, slack, sudden, head_gain, wo, out_gain):
        seg, model = tokens.shape[1:]
        hk = wq.shape[1]
        heads = hk // KEY
        features = wo.shape[1]
        rows_all = seg * n_tp
        block = min(128, seg)
        blocks = rows_all // block
        per_seg = seg // block
        groups = hk // 2 // KEY
        chips = n_sp // 2
        steps = max(1, (chips - 1).bit_length())
        peers = n_tp - 1
        any_spec = pl.BlockSpec(memory_space=pltpu.HBM)
        vmem = pl.BlockSpec(memory_space=pltpu.VMEM)
        dma = pltpu.SemaphoreType.DMA
        cfg = (n_sp, n_tp, seg, block, heads, model)
        call = pl.pallas_call(
            functools.partial(kernel, cfg),
            out_shape=pltpu.VMEM((rows_all, features), BF16),
            in_specs=[
                any_spec, vmem, any_spec, any_spec, any_spec, any_spec,
                vmem, vmem, vmem, any_spec, vmem,
            ],
            out_specs=vmem,
            scratch_shapes=[
                pltpu.VMEM((rows_all, model), BF16),
                pltpu.VMEM((4, model, hk), BF16),
                pltpu.VMEM((hk * n_tp, features), BF16),
                pltpu.VMEM((blocks, KEY, hk), F32),
                pltpu.VMEM((rows_all, hk), F32),
                pltpu.VMEM((rows_all, hk), BF16),
                pltpu.VMEM((rows_all, hk), F32),
                pltpu.VMEM((blocks, 8, hk), F32),
                pltpu.VMEM((blocks, 8, hk), F32),
                pltpu.VMEM((n_tp, groups, rows_all, 2 * KEY), BF16),
                pltpu.VMEM((rows_all, features), F32),
                pltpu.VMEM((rows_all, hk), F32),
                pltpu.VMEM((rows_all, hk), BF16),
                pltpu.VMEM((rows_all, hk), BF16),
                pltpu.VMEM((rows_all, model), BF16),
                pltpu.VMEM((KEY + 16, hk), BF16),
                pltpu.VMEM((KEY + 16, hk), BF16),
                pltpu.VMEM((steps, groups, KEY + 16, KEY), BF16),
                pltpu.VMEM((steps, groups, KEY + 16, KEY), BF16),
                pltpu.VMEM((groups, KEY, KEY), F32),
                pltpu.VMEM((groups, 8, KEY), F32),
                pltpu.VMEM((groups, KEY, KEY), F32),
                pltpu.VMEM((groups, 8, KEY), F32),
                pltpu.VMEM((groups, KEY, KEY), BF16),
                pltpu.VMEM((groups, KEY, KEY), BF16),
                pltpu.VMEM((KEY, 2 * KEY), F32),
                pltpu.VMEM((n_tp, blocks, 8, 128), F32),
                dma((4,)), dma((heads * n_tp,)), dma,
                dma((peers, per_seg)), dma((peers, per_seg)),
                dma, dma,
                dma((steps, groups)), dma((steps, groups)),
                dma((groups,)), dma((groups,)),
                dma((peers, groups, blocks)), dma((peers, groups, blocks)),
                dma((peers, blocks)), dma((peers, blocks)),
            ],
            compiler_params=pltpu.CompilerParams(
                collective_id=0, has_side_effects=True, vmem_limit_bytes=56 * 2**20
            ),
        )
        result = call(
            tokens[0], gain[None], wq, wf, wi, wg, slack[None], sudden[0].T,
            head_gain[None], wo, out_gain[None],
        )
        return result[None]

    placed = (
        P(None, ("sp", "tp"), None),
        P(),
        P(None, "tp"),
        P(None, "tp"),
        P(None, "tp"),
        P(None, "tp"),
        P("tp"),
        P(None, "sp", "tp"),
        P(),
        P(None, "tp"),
        P("tp"),
    )
    return jax.shard_map(
        shards, mesh=mesh, in_specs=placed, out_specs=P(None, "sp", "tp"), check_vma=False
    )
```
